32 devices in a mesh: fs: 16 (over z, y, x), tp: 2 (over core).
Axes of the slice: x: 2, y: 2, z: 4, core: 2. Of those that a mesh axis runs over, the one named last changes fastest.
Arguments:
- normed: bfloat16 [16384, 2048], P('fs'), may hold values from -6 to 6
- key_cot: bfloat16 [16384, 1024], P('fs', 'tp'), may hold values from -130 to 130
- value_cot: bfloat16 [16384, 2048], P('fs', 'tp'), may hold values from -130 to 130
- basis: bfloat16 [2048, 256], P('fs'), may hold values from -3.535534 to 3.535534
- master_key: float32 [2048, 1024], P('fs', 'tp'), may hold values from -3 to 3
- master_value: float32 [2048, 2048], P('fs', 'tp'), may hold values from -3 to 3
- first_key: float32 [256, 1024], P('fs', 'tp'), may hold values from -3 to 3
- second_key: float32 [256, 1024], P('fs', 'tp'), may hold values from 0.05 to 2
- first_value: float32 [256, 2048], P('fs', 'tp'), may hold values from -3 to 3
- second_value: float32 [256, 2048], P('fs', 'tp'), may hold values from 0.05 to 2
Outputs:
- step_key: float32 [2048, 1024], P('fs', 'tp')
- step_value: float32 [2048, 2048], P('fs', 'tp')
- new_master_key: float32 [2048, 1024], P('fs', 'tp')
- new_master_value: float32 [2048, 2048], P('fs', 'tp')
- copy_key: bfloat16 [2048, 1024], P(None, 'tp')
- copy_value: bfloat16 [2048, 2048], P(None, 'tp')
- new_first_key: float32 [256, 1024], P('fs', 'tp')
- new_second_key: float32 [256, 1024], P('fs', 'tp')
- new_first_value: float32 [256, 2048], P('fs', 'tp')
- new_second_value: float32 [256, 2048], P('fs', 'tp')
The draws below stay inside these ranges and needn't reach their ends.
All inputs are finite; a program needn't handle non-finite values.
Results may differ from the reference program's by a relative error of at most 0.0055.
Values may be sent and summed in bfloat16 or wider, within the bound.
No kernel may reach another device: no remote copies, remote signals or barrier semaphores. Data moves between devices by JAX's collectives and lax.ppermute only.
A program may use at most 64 MiB of HBM per device.

```python
import math
import jax
import jax.numpy as jnp
from jax import lax

D = 2048
DK = 1024
DV = 2048
R = 256
TOKENS = 16384


def column_scaled(key, height, width):
    keys = jax.random.split(key, 2)
    ramp = jnp.arange(width, dtype=jnp.float32) / max(width - 1, 1)
    jitter = jnp.exp(jax.random.uniform(keys[1], (width,), jnp.float32, math.log(0.7), math.log(1.4)))
    scales = 10.0 ** ramp * jitter
    base_values = jnp.clip(jax.random.normal(keys[0], (height, width), jnp.float32), -6.0, 6.0)
    return base_values * scales[None, :]


def draw_basis(key, part):
    values = column_scaled(jax.random.fold_in(key, 11), D, R) * D ** (-0.5)
    return values.astype(jnp.bfloat16)


def draw_key_cot(key, part):
    return column_scaled(jax.random.fold_in(key, 12), TOKENS, DK).astype(jnp.bfloat16)


def draw_value_cot(key, part):
    return column_scaled(jax.random.fold_in(key, 13), TOKENS, DV).astype(jnp.bfloat16)


def shard_levels(stream_key, dims, cuts, low, largest):
    factor_of, own = 1.0, jax.random.fold_in(stream_key, 6)
    for dim, blocks in cuts:
        steps = jnp.exp(jax.random.uniform(jax.random.fold_in(own, dim), (blocks,), jnp.float32, low / len(cuts), largest / len(cuts)))
        factor_of = factor_of * jnp.repeat(steps, dims[dim] // blocks).reshape([-1 if axis == dim else 1 for axis in range(len(dims))])
    return factor_of


def noise(stream_key, extent, deviation, limit, cuts=(), kind=jnp.bfloat16):
    gain = shard_levels(stream_key, extent, cuts, -0.22, 0.18) if cuts else 1.0
    drawn = jax.random.normal(stream_key, extent, jnp.float32) * deviation * gain
    return jnp.minimum(jnp.maximum(drawn, -limit), limit).astype(kind)


def setup_inputs(seed: int = 0) -> dict:
    arg_keys = jax.random.split(jax.random.key(seed), 11)
    return {
        "normed": noise(arg_keys[0], (TOKENS, D), 1.0, 6.0, ((0, 16),)),
        "key_cot": draw_key_cot(jax.random.fold_in(arg_keys[10], 71), 0),
        "value_cot": draw_value_cot(jax.random.fold_in(arg_keys[10], 71), 0),
        "basis": draw_basis(jax.random.fold_in(arg_keys[10], 71), 0),
        "master_key": noise(arg_keys[4], (D, DK), 0.5, 3.0, ((0, 16), (1, 2)), jnp.float32),
        "master_value": noise(arg_keys[5], (D, DV), 0.5, 3.0, ((0, 16), (1, 2)), jnp.float32),
        "first_key": noise(arg_keys[6], (R, DK), 0.5, 3.0, ((0, 16), (1, 2)), jnp.float32),
        "second_key": jnp.clip(jnp.exp(math.log(2.0) - 3.6888794 * jax.random.uniform(arg_keys[7], (R, DK), jnp.float32) ** shard_levels(arg_keys[7], (R, DK), ((0, 16), (1, 2)), -0.2, 0.2)), 0.05, 2.0),
        "first_value": noise(arg_keys[8], (R, DV), 0.5, 3.0, ((0, 16), (1, 2)), jnp.float32),
        "second_value": jnp.clip(jnp.exp(math.log(2.0) - 3.6888794 * jax.random.uniform(arg_keys[9], (R, DV), jnp.float32) ** shard_levels(arg_keys[9], (R, DV), ((0, 16), (1, 2)), -0.2, 0.2)), 0.05, 2.0),
    }


learn_rate = 0.05
beta_first = 0.9
beta_second = 0.9
epsilon = 1e-08
norm_eps = 1e-06

def moment_update(low_grad, grad_scale, first_moment, second_moment, basis):
    scaled = low_grad * grad_scale
    new_first = beta_first * first_moment + (1.0 - beta_first) * scaled
    new_second = beta_second * second_moment + (1.0 - beta_second) * scaled * scaled
    direction = (new_first / (jnp.sqrt(new_second) + epsilon)).astype(jnp.bfloat16)
    update_step = jnp.dot(basis, direction, preferred_element_type=jnp.float32)
    return (update_step, new_first, new_second)

def reference(normed, key_cot, value_cot, basis, master_key, master_value, first_key, second_key, first_value, second_value):
    grad_key = jnp.dot(normed.T, key_cot, preferred_element_type=jnp.float32)
    grad_value = jnp.dot(normed.T, value_cot, preferred_element_type=jnp.float32)
    basis_wide = basis.astype(jnp.float32).T
    low_key = jnp.dot(basis_wide, grad_key, precision=lax.Precision.HIGHEST, preferred_element_type=jnp.float32)
    low_value = jnp.dot(basis_wide, grad_value, precision=lax.Precision.HIGHEST, preferred_element_type=jnp.float32)
    squares = jnp.sum(low_key * low_key) + jnp.sum(low_value * low_value)
    root_mean = jnp.sqrt(squares / (R * (DK + DV)) + norm_eps)
    grad_scale = 1.0 / root_mean
    step_key, new_first_key, new_second_key = moment_update(low_key, grad_scale, first_key, second_key, basis)
    step_value, new_first_value, new_second_value = moment_update(low_value, grad_scale, first_value, second_value, basis)
    new_master_key = master_key - learn_rate * step_key
    new_master_value = master_value - learn_rate * step_value
    return (step_key, step_value, new_master_key, new_master_value, new_master_key.astype(jnp.bfloat16), new_master_value.astype(jnp.bfloat16), new_first_key, new_second_key, new_first_value, new_second_value)
```

```python
import functools

import jax
import jax.numpy as jnp
from jax import lax
from jax.experimental import pallas as pl
from jax.experimental.pallas import tpu as pltpu
from jax.sharding import PartitionSpec as P


learn_rate = 0.05
beta_first = 0.9
beta_second = 0.9
epsilon = 1e-08
norm_eps = 1e-06

INNER = 4


def swap(values, ranks, offset):
    return lax.ppermute(values, "fs", [(rank, rank ^ offset) for rank in range(ranks)])


def place(pieces, me, ranks, rows):
    whole = jnp.zeros((ranks * rows, pieces[0].shape[1]), pieces[0].dtype)
    for inner, column in enumerate(pieces):
        for outer in range(ranks // INNER):
            whole = lax.dynamic_update_slice_in_dim(
                whole, column[outer * rows : (outer + 1) * rows], (me ^ (outer * INNER + inner)) * rows, 0
            )
    return whole


def outer_column(block, ranks):
    pieces = [block] + [swap(block, ranks, INNER * step) for step in range(1, ranks // INNER)]
    return jnp.concatenate(pieces, axis=0)


def inner_gather(column, me, ranks, rows):
    column = lax.optimization_barrier(column)
    pieces = [column] + [swap(column, ranks, step) for step in range(1, INNER)]
    return place(pieces, me, ranks, rows)


def spread(block, ranks):
    last = ranks // INNER - 1
    chunks = []
    for chunk in range(last + 1):
        if chunk == last and chunk > 1:
            shard = swap(chunks[chunk - 1][1][0][2], ranks, INNER)
        else:
            shard = swap(block, ranks, INNER * chunk) if chunk else block
        first = swap(shard, ranks, 1)
        second = swap(shard, ranks, 2)
        if chunk == last:
            third = swap(shard, ranks, 3)
        elif chunk % 2:
            third = swap(first, ranks, 2)
        else:
            third = swap(second, ranks, 1)
        chunks.append((chunk, [(away, 0, part) for away, part in enumerate((shard, first, second, third))]))
    return chunks


def prepare_kernel(master_key, master_value, first_key, second_key, first_value, second_value, master, moments):
    key_cols = master_key.shape[1]
    cols = master.shape[1]
    master[:, :key_cols] = master_key[...].astype(jnp.bfloat16)
    master[:, key_cols:] = master_value[...].astype(jnp.bfloat16)
    moments[:, :key_cols] = first_key[...].astype(jnp.bfloat16)
    moments[:, key_cols:cols] = first_value[...].astype(jnp.bfloat16)
    moments[:, cols : cols + key_cols] = second_key[...].astype(jnp.bfloat16)
    moments[:, cols + key_cols :] = second_value[...].astype(jnp.bfloat16)


def prepare(master_key, master_value, first_key, second_key, first_value, second_value):
    cols = master_key.shape[1] + master_value.shape[1]
    return pl.pallas_call(
        prepare_kernel,
        out_shape=[
            jax.ShapeDtypeStruct((master_key.shape[0], cols), jnp.bfloat16),
            jax.ShapeDtypeStruct((first_key.shape[0], 2 * cols), jnp.bfloat16),
        ],
        name="prepare",
    )(master_key, master_value, first_key, second_key, first_value, second_value)


def gather_basis(basis, ranks):
    half = basis.shape[1] // 2
    others = lax.axis_size("tp")
    core = lax.axis_index("tp") % 2
    own = lax.dynamic_slice_in_dim(basis, core * half, half, 1)
    column = outer_column(own, ranks)
    mine = [column] + [swap(column, ranks, step) for step in range(1, INNER)]
    theirs = []
    for piece in mine:
        theirs.append(lax.ppermute(piece, "tp", [(rank, rank ^ 1) for rank in range(others)]))
    return mine, theirs


PARTS = 2


def project_kernel(groups, where, *refs):
    mine, theirs, refs = refs[:INNER], refs[INNER : 2 * INNER], refs[2 * INNER :]
    normed, key_cot, value_cot, whole_out, home, *aways = refs[: 5 + INNER - 1]
    tokens, cots, upper, whole, partial, home_buf, away_buf, token_sem, cot_sem, give_sem = refs[5 + INNER - 1 :]
    height = tokens.shape[0] // PARTS
    key_cols = key_cot.shape[1]
    loads = [
        pltpu.make_async_copy(
            normed.at[pl.ds(part * height, height)], tokens.at[pl.ds(part * height, height)], token_sem.at[part]
        )
        for part in range(PARTS)
    ]
    for load in loads:
        load.start()
    cot_loads = [
        pltpu.make_async_copy(key_cot, cots.at[:, pl.ds(0, key_cols)], cot_sem.at[0]),
        pltpu.make_async_copy(value_cot, cots.at[:, pl.ds(key_cols, value_cot.shape[1])], cot_sem.at[1]),
    ]
    for load in cot_loads:
        load.start()
    me, core = where[0], where[1]
    half = mine[0].shape[1]
    rows = mine[0].shape[0] // groups
    for first in range(2):

        @pl.when(core == first)
        def _(first=first):
            for away in range(INNER):
                for group in range(groups):
                    spot = pl.ds(pl.multiple_of((me ^ (group * INNER + away)) * rows, rows), rows)
                    part = slice(group * rows, (group + 1) * rows)
                    whole[spot, first * half : (first + 1) * half] = mine[away][part, :]
                    whole[spot, (1 - first) * half : (2 - first) * half] = theirs[away][part, :]

    gives = [pltpu.make_async_copy(whole, whole_out, give_sem.at[INNER])]
    gives[0].start()
    for part in range(PARTS):
        loads[part].wait()
        span = slice(part * height, (part + 1) * height)
        upper[span, :] = jnp.dot(tokens[span, :], whole[...], preferred_element_type=jnp.float32).astype(jnp.bfloat16)
    for load in cot_loads:
        load.wait()
    partial[...] = lax.dot_general(
        upper[...], cots[...], (((0,), (0,)), ((), ())), preferred_element_type=jnp.float32
    )
    if len(home.shape) == 2:
        gives.append(pltpu.make_async_copy(partial, home, give_sem.at[0]))
        gives[-1].start()
    else:
        low_rows = home.shape[1]
        for away in reversed(range(INNER)):
            for group in range(home.shape[0]):
                slot = group * INNER + ((me % INNER) ^ away)
                block = partial[pl.ds(pl.multiple_of(slot * low_rows, low_rows), low_rows), :]
                if away:
                    away_buf[away - 1, group] = block.astype(jnp.bfloat16)
                else:
                    home_buf[group] = block
            source, target = (away_buf.at[away - 1], aways[away - 1]) if away else (home_buf, home)
            gives.append(pltpu.make_async_copy(source, target, give_sem.at[away]))
            gives[-1].start()
    for give in gives:
        give.wait()


def project(mine, theirs, normed, key_cot, value_cot, me, ranks):
    depth = 2 * mine[0].shape[1]
    groups = ranks // INNER
    low_rows = depth // ranks
    cols = key_cot.shape[1] + value_cot.shape[1]
    where = jnp.stack([me, lax.axis_index("tp") % 2]).astype(jnp.int32)
    local = pl.BlockSpec(memory_space=pltpu.VMEM)
    anywhere = pl.BlockSpec(memory_space=pl.ANY)
    tidy = low_rows % 8 == 0
    home = jax.ShapeDtypeStruct((groups, low_rows, cols) if tidy else (depth, cols), jnp.float32)
    away = jax.ShapeDtypeStruct((groups, low_rows, cols) if tidy else (8, 128), jnp.bfloat16)
    whole, home, *aways = pl.pallas_call(
        functools.partial(project_kernel, groups),
        in_specs=[pl.BlockSpec(memory_space=pltpu.SMEM)] + [local] * (2 * INNER) + [anywhere] * 3,
        out_specs=[anywhere] * 2 + [anywhere if tidy else local] * (INNER - 1),
        out_shape=[jax.ShapeDtypeStruct((normed.shape[1], depth), jnp.bfloat16), home] + [away] * (INNER - 1),
        scratch_shapes=[
            pltpu.VMEM(normed.shape, jnp.bfloat16),
            pltpu.VMEM((normed.shape[0], cols), jnp.bfloat16),
            pltpu.VMEM((normed.shape[0], depth), jnp.bfloat16),
            pltpu.VMEM((normed.shape[1], depth), jnp.bfloat16),
            pltpu.VMEM((depth, cols), jnp.float32),
            pltpu.VMEM((groups, low_rows, cols), jnp.float32),
            pltpu.VMEM((INNER - 1, groups, low_rows, cols), jnp.bfloat16),
            pltpu.SemaphoreType.DMA((PARTS,)),
            pltpu.SemaphoreType.DMA((2,)),
            pltpu.SemaphoreType.DMA((INNER + 1,)),
        ],
        name="project",
    )(where, *mine, *theirs, normed, key_cot, value_cot)
    if not tidy:
        blocks = home.reshape(groups, INNER, low_rows, cols)
        inner = me % INNER
        home = lax.dynamic_index_in_dim(blocks, inner, 1, keepdims=False)
        aways = [
            lax.dynamic_index_in_dim(blocks, inner ^ step, 1, keepdims=False).astype(jnp.bfloat16)
            for step in range(1, INNER)
        ]
    return whole, home, aways


def scatter_sum(total, aways, me, ranks):
    groups = ranks // INNER
    for step, away in enumerate(aways, 1):
        total = total + swap(away, ranks, step).astype(jnp.float32)
    high = me // INNER
    own = lax.dynamic_index_in_dim(total, high, 0, keepdims=False)
    for step in range(1, groups):
        away = lax.dynamic_index_in_dim(total, high ^ step, 0, keepdims=False).astype(jnp.bfloat16)
        own = own + swap(away, ranks, step * INNER).astype(jnp.float32)
    return own


def pair_sum(parts):
    while len(parts) > 1:
        parts = [left + right for left, right in zip(parts[::2], parts[1::2])]
    return parts[0]


def sum_everywhere(rows_of, ranks):
    value = pair_sum([jnp.sum((part * part).reshape(part.shape[0], -1, 128), axis=1) for part in rows_of])
    received = [swap(value, ranks, step) for step in range(1, INNER)]
    value = pair_sum([value] + received)
    others = lax.axis_size("tp")
    total = value
    for step in range(1, others):
        total = total + lax.ppermute(value, "tp", [(rank, (rank + step) % others) for rank in range(others)])
    return jnp.sum(total)


def copy_kernel(layout, with_own, inherited, *refs):
    count = sum(len(parts) for _, parts in layout)
    order, basis, directions, *rest = refs
    pieces, rest = rest[:count], rest[count:]
    masters, rest = (rest[:2], rest[2:]) if with_own else ((), rest)
    rest = rest[inherited:]
    copy_key, copy_value, *rest = rest
    results, rest = (rest[:4], rest[4:]) if with_own else ((), rest)
    taken, made, step, take_sem, key_sem, value_sem, *rest = rest
    rows = step.shape[0] // INNER
    key_cols = copy_key.shape[1]
    here = order[0]
    inner = here % INNER
    outer = here // INNER
    takes = [
        pltpu.make_async_copy(piece, taken.at[slot, pl.ds(0, piece.shape[0])], take_sem.at[slot])
        for slot, piece in enumerate(pieces)
    ]
    for take in takes:
        take.start()
    if with_own:
        own_key, own_value, own_step, own_take, own_give = rest
        own_takes = [
            pltpu.make_async_copy(masters[0], own_key, own_take.at[0]),
            pltpu.make_async_copy(masters[1], own_value, own_take.at[1]),
        ]
        for take in own_takes:
            take.start()
    gives = []
    slot = 0
    for chunk, parts in layout:
        first_row = pl.multiple_of((outer ^ chunk) * INNER * rows, INNER * rows)
        if len(parts) == INNER:
            step[...] = jnp.dot(
                basis[pl.ds(first_row, INNER * rows), :], directions[...], preferred_element_type=jnp.float32
            )
        for away, start in parts:
            size = pieces[slot].shape[0]
            spot = pl.multiple_of((inner ^ away) * rows + start, size)
            if len(parts) != INNER:
                step[pl.ds(spot, size), :] = jnp.dot(
                    basis[pl.ds(pl.multiple_of(first_row + spot, size), size), :],
                    directions[...],
                    preferred_element_type=jnp.float32,
                )
            takes[slot].wait()
            change = learn_rate * step[pl.ds(spot, size), :]
            made[slot, pl.ds(0, size)] = (taken[slot, pl.ds(0, size)].astype(jnp.float32) - change).astype(jnp.bfloat16)
            target = pl.ds(pl.multiple_of(first_row + spot, size), size)
            for out_ref, columns, sem in (
                (copy_key, pl.ds(0, key_cols), key_sem),
                (copy_value, pl.ds(key_cols, step.shape[1] - key_cols), value_sem),
            ):
                give = pltpu.make_async_copy(
                    made.at[slot, pl.ds(0, size), columns], out_ref.at[target, :], sem.at[slot]
                )
                give.start()
                gives.append(give)
            slot += 1
        if with_own and chunk == 0:
            for take in own_takes:
                take.wait()
            own_step[...] = step[pl.ds(pl.multiple_of(inner * rows, rows), rows), :]
            own_key[...] = own_key[...] - learn_rate * own_step[:, :key_cols]
            own_value[...] = own_value[...] - learn_rate * own_step[:, key_cols:]
            value_cols = step.shape[1] - key_cols
            for place_in, (source, target) in enumerate(
                (
                    (own_step.at[:, pl.ds(0, key_cols)], results[0]),
                    (own_step.at[:, pl.ds(key_cols, value_cols)], results[1]),
                    (own_key, results[2]),
                    (own_value, results[3]),
                )
            ):
                give = pltpu.make_async_copy(source, target, own_give.at[place_in])
                give.start()
                gives.append(give)
    for give in gives:
        give.wait()


def write_copies(chunks, masters, me, basis, directions, key_cols, ranks, earlier):
    rows = basis.shape[0] // ranks
    cols = directions.shape[1]
    layout = tuple((chunk, tuple((away, start) for away, start, _ in parts)) for chunk, parts in chunks)
    pieces = [part for _, parts in chunks for _, _, part in parts]
    count = len(pieces)
    tallest = max(piece.shape[0] for piece in pieces)
    anywhere = pl.BlockSpec(memory_space=pl.ANY)
    local = pl.BlockSpec(memory_space=pltpu.VMEM)
    out_shape = [
        jax.ShapeDtypeStruct((ranks * rows, key_cols), jnp.bfloat16),
        jax.ShapeDtypeStruct((ranks * rows, cols - key_cols), jnp.bfloat16),
    ]
    scratch = [
        pltpu.VMEM((count, tallest, cols), jnp.bfloat16),
        pltpu.VMEM((count, tallest, cols), jnp.bfloat16),
        pltpu.VMEM((INNER * rows, cols), jnp.float32),
        pltpu.SemaphoreType.DMA((count,)),
        pltpu.SemaphoreType.DMA((count,)),
        pltpu.SemaphoreType.DMA((count,)),
    ]
    if masters:
        out_shape += [jax.ShapeDtypeStruct(master.shape, jnp.float32) for master in (*masters, *masters)]
        scratch += [
            pltpu.VMEM(masters[0].shape, jnp.float32),
            pltpu.VMEM(masters[1].shape, jnp.float32),
            pltpu.VMEM((rows, cols), jnp.float32),
            pltpu.SemaphoreType.DMA((2,)),
            pltpu.SemaphoreType.DMA((4,)),
        ]
    first_alias = 3 + count + len(masters)
    return pl.pallas_call(
        functools.partial(copy_kernel, layout, bool(masters), len(earlier)),
        in_specs=[pl.BlockSpec(memory_space=pltpu.SMEM), local, local]
        + [anywhere] * (count + len(masters) + len(earlier)),
        out_specs=[anywhere] * len(out_shape),
        out_shape=out_shape,
        scratch_shapes=scratch,
        input_output_aliases={first_alias: 0, first_alias + 1: 1} if earlier else {},
    )(me.reshape(1), basis, directions, *pieces, *masters, *earlier)


def on_device(
    total_count,
    ranks,
    normed,
    key_cot,
    value_cot,
    basis,
    master_key,
    master_value,
    first_key,
    second_key,
    first_value,
    second_value,
):
    me = lax.axis_index("fs")
    key_cols = key_cot.shape[1]
    mine, theirs = gather_basis(basis, ranks)
    master, moments_sent = prepare(master_key, master_value, first_key, second_key, first_value, second_value)
    chunks = spread(master, ranks)
    moments = outer_column(moments_sent, ranks).astype(jnp.float32)
    whole_basis, home, aways = project(mine, theirs, normed, key_cot, value_cot, me, ranks)
    low = scatter_sum(home, aways, me, ranks)
    low_column = outer_column(low.astype(jnp.bfloat16), ranks).astype(jnp.float32)
    height = low.shape[0]
    squares = sum_everywhere(
        [low_column[start : start + height] for start in range(0, low_column.shape[0], height)], ranks
    )
    grad_scale = 1.0 / jnp.sqrt(squares / total_count + norm_eps)

    def advance(low_part, first, second):
        scaled = low_part * grad_scale
        new_first = beta_first * first + (1.0 - beta_first) * scaled
        new_second = beta_second * second + (1.0 - beta_second) * scaled * scaled
        return new_first, new_second

    cols = low.shape[1]
    new_first, new_second = advance(low_column, moments[:, :cols], moments[:, cols:])
    direction = (new_first / (jnp.sqrt(new_second) + epsilon)).astype(jnp.bfloat16)
    directions = inner_gather(direction, me, ranks, low.shape[0])
    first_key, second_key, first_value, second_value, low = lax.optimization_barrier(
        (first_key, second_key, first_value, second_value, low)
    )
    new_first_key, new_second_key = advance(low[:, :key_cols], first_key, second_key)
    new_first_value, new_second_value = advance(low[:, key_cols:], first_value, second_value)
    copy_key, copy_value, *own = write_copies(
        chunks[:-1], (master_key, master_value), me, whole_basis, directions, key_cols, ranks, ()
    )
    copy_key, copy_value = write_copies(
        chunks[-1:], (), me, whole_basis, directions, key_cols, ranks, (copy_key, copy_value)
    )
    return (*own, copy_key, copy_value, new_first_key, new_second_key, new_first_value, new_second_value)


def solution(mesh):
    split = P("fs", "tp")
    rows = P("fs", None)
    ranks = mesh.shape["fs"]
    tensor = mesh.shape["tp"]

    def body(*arguments):
        first_key, first_value = arguments[6], arguments[8]
        count = ranks * tensor * (first_key.size + first_value.size)
        return on_device(count, ranks, *arguments)

    return jax.shard_map(
        body,
        mesh=mesh,
        in_specs=(rows, split, split, rows) + (split,) * 6,
        out_specs=(split,) * 4 + (P(None, "tp"),) * 2 + (split,) * 4,
        check_vma=False,
    )
```

```python
import functools

import jax
import jax.numpy as jnp
from jax import lax
from jax.experimental import pallas as pl
from jax.experimental.pallas import tpu as pltpu
from jax.sharding import PartitionSpec as P


learn_rate = 0.05
beta_first = 0.9
beta_second = 0.9
epsilon = 1e-08
norm_eps = 1e-06

INNER = 4


def swap(values, ranks, offset):
    return lax.ppermute(values, "fs", [(rank, rank ^ offset) for rank in range(ranks)])


def place(pieces, me, ranks, rows):
    whole = jnp.zeros((ranks * rows, pieces[0].shape[1]), pieces[0].dtype)
    for inner, column in enumerate(pieces):
        for outer in range(ranks // INNER):
            whole = lax.dynamic_update_slice_in_dim(
                whole, column[outer * rows : (outer + 1) * rows], (me ^ (outer * INNER + inner)) * rows, 0
            )
    return whole


def outer_column(block, ranks):
    pieces = [block] + [swap(block, ranks, INNER * step) for step in range(1, ranks // INNER)]
    return jnp.concatenate(pieces, axis=0)


def inner_gather(column, me, ranks, rows):
    column = lax.optimization_barrier(column)
    pieces = [column] + [swap(column, ranks, step) for step in range(1, INNER)]
    return place(pieces, me, ranks, rows)


def spread(block, ranks):
    last = ranks // INNER - 1
    chunks = []
    for chunk in range(last + 1):
        if chunk == last and chunk > 1:
            shard = swap(chunks[chunk - 1][1][0][2], ranks, INNER)
        else:
            shard = swap(block, ranks, INNER * chunk) if chunk else block
        first = swap(shard, ranks, 1)
        second = swap(shard, ranks, 2)
        if chunk == last:
            third = swap(shard, ranks, 3)
        elif chunk % 2:
            third = swap(first, ranks, 2)
        else:
            third = swap(second, ranks, 1)
        chunks.append((chunk, [(away, 0, part) for away, part in enumerate((shard, first, second, third))]))
    return chunks


def in_vmem(*arrays):
    return [pltpu.with_memory_space_constraint(array, pltpu.VMEM) for array in arrays]


def prepare_kernel(master_key, master_value, first_key, second_key, first_value, second_value, master, moments):
    key_cols = master_key.shape[1]
    cols = master.shape[1]
    master[:, :key_cols] = master_key[...].astype(jnp.bfloat16)
    master[:, key_cols:] = master_value[...].astype(jnp.bfloat16)
    moments[:, :key_cols] = first_key[...].astype(jnp.bfloat16)
    moments[:, key_cols:cols] = first_value[...].astype(jnp.bfloat16)
    moments[:, cols : cols + key_cols] = second_key[...].astype(jnp.bfloat16)
    moments[:, cols + key_cols :] = second_value[...].astype(jnp.bfloat16)


def prepare(master_key, master_value, first_key, second_key, first_value, second_value):
    cols = master_key.shape[1] + master_value.shape[1]
    return pl.pallas_call(
        prepare_kernel,
        out_shape=[
            jax.ShapeDtypeStruct((master_key.shape[0], cols), jnp.bfloat16),
            jax.ShapeDtypeStruct((first_key.shape[0], 2 * cols), jnp.bfloat16),
        ],
        name="prepare",
    )(master_key, master_value, first_key, second_key, first_value, second_value)


def gather_basis(basis, ranks):
    half = basis.shape[1] // 2
    others = lax.axis_size("tp")
    core = lax.axis_index("tp") % 2
    own = lax.dynamic_slice_in_dim(basis, core * half, half, 1)
    column = outer_column(own, ranks)
    mine = [column] + [swap(column, ranks, step) for step in range(1, INNER)]
    theirs = []
    for piece in mine:
        theirs.append(lax.ppermute(piece, "tp", [(rank, rank ^ 1) for rank in range(others)]))
    return mine, theirs


PARTS = 4


def project_kernel(groups, *refs):
    mine, theirs, refs = refs[:INNER], refs[INNER : 2 * INNER], refs[2 * INNER :]
    normed, key_cot, value_cot, whole_out, home, *aways = refs[: 5 + INNER - 1]
    tokens, cots, upper, whole, partial, home_buf, away_buf, token_sem, cot_sem, give_sem = refs[5 + INNER - 1 :]
    height = tokens.shape[0] // PARTS
    key_cols = key_cot.shape[1]
    loads = [
        pltpu.make_async_copy(
            normed.at[pl.ds(part * height, height)], tokens.at[pl.ds(part * height, height)], token_sem.at[part]
        )
        for part in range(PARTS)
    ]
    for load in loads:
        load.start()
    cot_loads = [
        pltpu.make_async_copy(key_cot, cots.at[:, pl.ds(0, key_cols)], cot_sem.at[0]),
        pltpu.make_async_copy(value_cot, cots.at[:, pl.ds(key_cols, value_cot.shape[1])], cot_sem.at[1]),
    ]
    for load in cot_loads:
        load.start()
    me, core = lax.axis_index("fs"), lax.axis_index("tp") % 2
    half = mine[0].shape[1]
    rows = mine[0].shape[0] // groups
    for first in range(2):

        @pl.when(core == first)
        def _(first=first):
            for away in range(INNER):
                for group in range(groups):
                    spot = pl.ds(pl.multiple_of((me ^ (group * INNER + away)) * rows, rows), rows)
                    part = slice(group * rows, (group + 1) * rows)
                    whole[spot, first * half : (first + 1) * half] = mine[away][part, :]
                    whole[spot, (1 - first) * half : (2 - first) * half] = theirs[away][part, :]

    gives = [pltpu.make_async_copy(whole, whole_out, give_sem.at[INNER])]
    gives[0].start()
    for part in range(PARTS):
        loads[part].wait()
        span = slice(part * height, (part + 1) * height)
        upper[span, :] = jnp.dot(tokens[span, :], whole[...], preferred_element_type=jnp.float32).astype(jnp.bfloat16)
    for load in cot_loads:
        load.wait()
    partial[...] = lax.dot_general(
        upper[...], cots[...], (((0,), (0,)), ((), ())), preferred_element_type=jnp.float32
    )
    if len(home.shape) == 2:
        gives.append(pltpu.make_async_copy(partial, home, give_sem.at[0]))
        gives[-1].start()
    else:
        low_rows = home.shape[1]
        for away in reversed(range(INNER)):
            for group in range(home.shape[0]):
                slot = group * INNER + ((me % INNER) ^ away)
                block = partial[pl.ds(pl.multiple_of(slot * low_rows, low_rows), low_rows), :]
                if away:
                    away_buf[away - 1, group] = block.astype(jnp.bfloat16)
                else:
                    home_buf[group] = block
            source, target = (away_buf.at[away - 1], aways[away - 1]) if away else (home_buf, home)
            gives.append(pltpu.make_async_copy(source, target, give_sem.at[away]))
            gives[-1].start()
    for give in gives:
        give.wait()


def project(mine, theirs, normed, key_cot, value_cot, me, ranks):
    depth = 2 * mine[0].shape[1]
    groups = ranks // INNER
    low_rows = depth // ranks
    cols = key_cot.shape[1] + value_cot.shape[1]
    local = pl.BlockSpec(memory_space=pltpu.VMEM)
    anywhere = pl.BlockSpec(memory_space=pl.ANY)
    tidy = low_rows % 8 == 0
    home = jax.ShapeDtypeStruct((groups, low_rows, cols) if tidy else (depth, cols), jnp.float32)
    away = jax.ShapeDtypeStruct((groups, low_rows, cols) if tidy else (8, 128), jnp.bfloat16)
    whole, home, *aways = pl.pallas_call(
        functools.partial(project_kernel, groups),
        in_specs=[local] * (2 * INNER) + [anywhere] * 3,
        out_specs=[anywhere] * 2 + [anywhere if tidy else local] * (INNER - 1),
        out_shape=[jax.ShapeDtypeStruct((normed.shape[1], depth), jnp.bfloat16), home] + [away] * (INNER - 1),
        scratch_shapes=[
            pltpu.VMEM(normed.shape, jnp.bfloat16),
            pltpu.VMEM((normed.shape[0], cols), jnp.bfloat16),
            pltpu.VMEM((normed.shape[0], depth), jnp.bfloat16),
            pltpu.VMEM((normed.shape[1], depth), jnp.bfloat16),
            pltpu.VMEM((depth, cols), jnp.float32),
            pltpu.VMEM((groups, low_rows, cols), jnp.float32),
            pltpu.VMEM((INNER - 1, groups, low_rows, cols), jnp.bfloat16),
            pltpu.SemaphoreType.DMA((PARTS,)),
            pltpu.SemaphoreType.DMA((2,)),
            pltpu.SemaphoreType.DMA((INNER + 1,)),
        ],
        name="project",
    )(*in_vmem(*mine, *theirs), normed, key_cot, value_cot)
    if not tidy:
        blocks = home.reshape(groups, INNER, low_rows, cols)
        inner = me % INNER
        home = lax.dynamic_index_in_dim(blocks, inner, 1, keepdims=False)
        aways = [
            lax.dynamic_index_in_dim(blocks, inner ^ step, 1, keepdims=False).astype(jnp.bfloat16)
            for step in range(1, INNER)
        ]
    return whole, home, aways


def scatter_sum(total, aways, me, ranks):
    groups = ranks // INNER
    for step, away in enumerate(aways, 1):
        total = total + swap(away, ranks, step).astype(jnp.float32)
    high = me // INNER
    own = lax.dynamic_index_in_dim(total, high, 0, keepdims=False)
    for step in range(1, groups):
        away = lax.dynamic_index_in_dim(total, high ^ step, 0, keepdims=False).astype(jnp.bfloat16)
        own = own + swap(away, ranks, step * INNER).astype(jnp.float32)
    return own


def pair_sum(parts):
    while len(parts) > 1:
        parts = [left + right for left, right in zip(parts[::2], parts[1::2])]
    return parts[0]


def sum_everywhere(rows_of, ranks):
    value = pair_sum([jnp.sum((part * part).reshape(part.shape[0], -1, 128), axis=1) for part in rows_of])
    received = [swap(value, ranks, step) for step in range(1, INNER)]
    value = pair_sum([value] + received)
    others = lax.axis_size("tp")
    total = value
    for step in range(1, others):
        total = total + lax.ppermute(value, "tp", [(rank, (rank + step) % others) for rank in range(others)])
    return jnp.sum(total)


def copy_kernel(layout, with_own, inherited, *refs):
    count = sum(len(parts) for _, parts in layout)
    basis, directions, *rest = refs
    pieces, rest = rest[:count], rest[count:]
    masters, rest = (rest[:2], rest[2:]) if with_own else ((), rest)
    rest = rest[inherited:]
    copy_key, copy_value, *rest = rest
    results, rest = (rest[:4], rest[4:]) if with_own else ((), rest)
    taken, made, step, take_sem, key_sem, value_sem, *rest = rest
    rows = step.shape[0] // INNER
    key_cols = copy_key.shape[1]
    here = lax.axis_index("fs")
    inner = here % INNER
    outer = here // INNER
    takes = []
    if with_own:
        takes = [
            pltpu.make_async_copy(piece, taken.at[slot, pl.ds(0, piece.shape[0])], take_sem.at[slot])
            for slot, piece in enumerate(pieces)
        ]
    for take in takes:
        take.start()
    if with_own:
        own_key, own_value, own_step, own_take, own_give = rest
        own_takes = [
            pltpu.make_async_copy(masters[0], own_key, own_take.at[0]),
            pltpu.make_async_copy(masters[1], own_value, own_take.at[1]),
        ]
        for take in own_takes:
            take.start()
    gives = []
    slot = 0
    for chunk, parts in layout:
        first_row = pl.multiple_of((outer ^ chunk) * INNER * rows, INNER * rows)
        if len(parts) == INNER:
            step[...] = jnp.dot(
                basis[pl.ds(first_row, INNER * rows), :], directions[...], preferred_element_type=jnp.float32
            )
        for away, start in parts:
            size = pieces[slot].shape[0]
            spot = pl.multiple_of((inner ^ away) * rows + start, size)
            if len(parts) != INNER:
                step[pl.ds(spot, size), :] = jnp.dot(
                    basis[pl.ds(pl.multiple_of(first_row + spot, size), size), :],
                    directions[...],
                    preferred_element_type=jnp.float32,
                )
            if takes:
                takes[slot].wait()
                piece = taken[slot, pl.ds(0, size)]
            else:
                piece = pieces[slot][...]
            change = learn_rate * step[pl.ds(spot, size), :]
            made[slot, pl.ds(0, size)] = (piece.astype(jnp.float32) - change).astype(jnp.bfloat16)
            target = pl.ds(pl.multiple_of(first_row + spot, size), size)
            for out_ref, columns, sem in (
                (copy_key, pl.ds(0, key_cols), key_sem),
                (copy_value, pl.ds(key_cols, step.shape[1] - key_cols), value_sem),
            ):
                give = pltpu.make_async_copy(
                    made.at[slot, pl.ds(0, size), columns], out_ref.at[target, :], sem.at[slot]
                )
                give.start()
                gives.append(give)
            slot += 1
        if with_own and chunk == 0:
            for take in own_takes:
                take.wait()
            own_step[...] = step[pl.ds(pl.multiple_of(inner * rows, rows), rows), :]
            own_key[...] = own_key[...] - learn_rate * own_step[:, :key_cols]
            own_value[...] = own_value[...] - learn_rate * own_step[:, key_cols:]
            value_cols = step.shape[1] - key_cols
            for place_in, (source, target) in enumerate(
                (
                    (own_step.at[:, pl.ds(0, key_cols)], results[0]),
                    (own_step.at[:, pl.ds(key_cols, value_cols)], results[1]),
                    (own_key, results[2]),
                    (own_value, results[3]),
                )
            ):
                give = pltpu.make_async_copy(source, target, own_give.at[place_in])
                give.start()
                gives.append(give)
    for give in gives:
        give.wait()


def write_copies(chunks, masters, basis, directions, key_cols, ranks, earlier):
    rows = basis.shape[0] // ranks
    cols = directions.shape[1]
    layout = tuple((chunk, tuple((away, start) for away, start, _ in parts)) for chunk, parts in chunks)
    pieces = [part for _, parts in chunks for _, _, part in parts]
    count = len(pieces)
    tallest = max(piece.shape[0] for piece in pieces)
    anywhere = pl.BlockSpec(memory_space=pl.ANY)
    local = pl.BlockSpec(memory_space=pltpu.VMEM)
    out_shape = [
        jax.ShapeDtypeStruct((ranks * rows, key_cols), jnp.bfloat16),
        jax.ShapeDtypeStruct((ranks * rows, cols - key_cols), jnp.bfloat16),
    ]
    scratch = [
        pltpu.VMEM((count, tallest, cols), jnp.bfloat16),
        pltpu.VMEM((count, tallest, cols), jnp.bfloat16),
        pltpu.VMEM((INNER * rows, cols), jnp.float32),
        pltpu.SemaphoreType.DMA((count,)),
        pltpu.SemaphoreType.DMA((count,)),
        pltpu.SemaphoreType.DMA((count,)),
    ]
    if masters:
        out_shape += [jax.ShapeDtypeStruct(master.shape, jnp.float32) for master in (*masters, *masters)]
        scratch += [
            pltpu.VMEM(masters[0].shape, jnp.float32),
            pltpu.VMEM(masters[1].shape, jnp.float32),
            pltpu.VMEM((rows, cols), jnp.float32),
            pltpu.SemaphoreType.DMA((2,)),
            pltpu.SemaphoreType.DMA((4,)),
        ]
    first_alias = 2 + count + len(masters)
    return pl.pallas_call(
        functools.partial(copy_kernel, layout, bool(masters), len(earlier)),
        in_specs=[local, local]
        + [anywhere if masters else local] * count
        + [anywhere] * (len(masters) + len(earlier)),
        out_specs=[anywhere] * len(out_shape),
        out_shape=out_shape,
        scratch_shapes=scratch,
        input_output_aliases={first_alias: 0, first_alias + 1: 1} if earlier else {},
    )(basis, *in_vmem(directions), *(pieces if masters else in_vmem(*pieces)), *masters, *earlier)


def on_device(
    total_count,
    ranks,
    normed,
    key_cot,
    value_cot,
    basis,
    master_key,
    master_value,
    first_key,
    second_key,
    first_value,
    second_value,
):
    me = lax.axis_index("fs")
    key_cols = key_cot.shape[1]
    mine, theirs = gather_basis(basis, ranks)
    master, moments_sent = prepare(master_key, master_value, first_key, second_key, first_value, second_value)
    chunks = spread(master, ranks)
    moments = outer_column(moments_sent, ranks).astype(jnp.float32)
    whole_basis, home, aways = project(mine, theirs, normed, key_cot, value_cot, me, ranks)
    low = scatter_sum(home, aways, me, ranks)
    low_column = outer_column(low.astype(jnp.bfloat16), ranks).astype(jnp.float32)
    height = low.shape[0]
    squares = sum_everywhere(
        [low_column[start : start + height] for start in range(0, low_column.shape[0], height)], ranks
    )
    grad_scale = 1.0 / jnp.sqrt(squares / total_count + norm_eps)

    def advance(low_part, first, second):
        scaled = low_part * grad_scale
        new_first = beta_first * first + (1.0 - beta_first) * scaled
        new_second = beta_second * second + (1.0 - beta_second) * scaled * scaled
        return new_first, new_second

    cols = low.shape[1]
    new_first, new_second = advance(low_column, moments[:, :cols], moments[:, cols:])
    direction = (new_first / (jnp.sqrt(new_second) + epsilon)).astype(jnp.bfloat16)
    directions = inner_gather(direction, me, ranks, low.shape[0])
    first_key, second_key, first_value, second_value, low = lax.optimization_barrier(
        (first_key, second_key, first_value, second_value, low)
    )
    new_first_key, new_second_key = advance(low[:, :key_cols], first_key, second_key)
    new_first_value, new_second_value = advance(low[:, key_cols:], first_value, second_value)
    copy_key, copy_value, *own = write_copies(
        chunks[:-1], (master_key, master_value), whole_basis, directions, key_cols, ranks, ()
    )
    copy_key, copy_value = write_copies(
        chunks[-1:], (), whole_basis, directions, key_cols, ranks, (copy_key, copy_value)
    )
    return (*own, copy_key, copy_value, new_first_key, new_second_key, new_first_value, new_second_value)


def solution(mesh):
    split = P("fs", "tp")
    rows = P("fs", None)
    ranks = mesh.shape["fs"]
    tensor = mesh.shape["tp"]

    def body(*arguments):
        first_key, first_value = arguments[6], arguments[8]
        count = ranks * tensor * (first_key.size + first_value.size)
        return on_device(count, ranks, *arguments)

    return jax.shard_map(
        body,
        mesh=mesh,
        in_specs=(rows, split, split, rows) + (split,) * 6,
        out_specs=(split,) * 4 + (P(None, "tp"),) * 2 + (split,) * 4,
        check_vma=False,
    )
```

```python
import functools

import jax
import jax.numpy as jnp
from jax import lax
from jax.experimental import pallas as pl
from jax.experimental.pallas import tpu as pltpu
from jax.sharding import PartitionSpec as P


learn_rate = 0.05
beta_first = 0.9
beta_second = 0.9
epsilon = 1e-08
norm_eps = 1e-06

INNER = 4


def swap(values, ranks, offset):
    return lax.ppermute(values, "fs", [(rank, rank ^ offset) for rank in range(ranks)])


def place(pieces, me, ranks, rows):
    whole = jnp.zeros((ranks * rows, pieces[0].shape[1]), pieces[0].dtype)
    for inner, column in enumerate(pieces):
        for outer in range(ranks // INNER):
            whole = lax.dynamic_update_slice_in_dim(
                whole, column[outer * rows : (outer + 1) * rows], (me ^ (outer * INNER + inner)) * rows, 0
            )
    return whole


def outer_column(block, ranks):
    pieces = [block] + [swap(block, ranks, INNER * step) for step in range(1, ranks // INNER)]
    return jnp.concatenate(pieces, axis=0)


def inner_gather(column, me, ranks, rows):
    column = lax.optimization_barrier(column)
    pieces = [column] + [swap(column, ranks, step) for step in range(1, INNER)]
    return place(pieces, me, ranks, rows)


def spread(block, ranks):
    last = ranks // INNER - 1
    chunks = []
    for chunk in range(last + 1):
        if chunk == last and chunk > 1:
            shard = swap(chunks[chunk - 1][1][0][2], ranks, INNER)
        else:
            shard = swap(block, ranks, INNER * chunk) if chunk else block
        first = swap(shard, ranks, 1)
        second = swap(shard, ranks, 2)
        if chunk == last:
            half = shard.shape[0] // 2
            top = swap(second[:half], ranks, 1)
            bottom = swap(first[half:], ranks, 2)
            chunks.append((chunk, [(0, 0, shard), (1, 0, first), (2, 0, second), (3, 0, top), (3, half, bottom)]))
            continue
        third = swap(first, ranks, 2) if chunk % 2 else swap(second, ranks, 1)
        chunks.append((chunk, [(away, 0, part) for away, part in enumerate((shard, first, second, third))]))
    return chunks


def in_vmem(*arrays):
    return [pltpu.with_memory_space_constraint(array, pltpu.VMEM) for array in arrays]


def prepare_kernel(master_key, master_value, first_key, second_key, first_value, second_value, master, moments):
    key_cols = master_key.shape[1]
    cols = master.shape[1]
    master[:, :key_cols] = master_key[...].astype(jnp.bfloat16)
    master[:, key_cols:] = master_value[...].astype(jnp.bfloat16)
    moments[:, :key_cols] = first_key[...].astype(jnp.bfloat16)
    moments[:, key_cols:cols] = first_value[...].astype(jnp.bfloat16)
    moments[:, cols : cols + key_cols] = second_key[...].astype(jnp.bfloat16)
    moments[:, cols + key_cols :] = second_value[...].astype(jnp.bfloat16)


def prepare(master_key, master_value, first_key, second_key, first_value, second_value):
    cols = master_key.shape[1] + master_value.shape[1]
    return pl.pallas_call(
        prepare_kernel,
        out_shape=[
            jax.ShapeDtypeStruct((master_key.shape[0], cols), jnp.bfloat16),
            jax.ShapeDtypeStruct((first_key.shape[0], 2 * cols), jnp.bfloat16),
        ],
        name="prepare",
    )(master_key, master_value, first_key, second_key, first_value, second_value)


def gather_basis(basis, ranks):
    half = basis.shape[1] // 2
    others = lax.axis_size("tp")
    core = lax.axis_index("tp") % 2
    own = lax.dynamic_slice_in_dim(basis, core * half, half, 1)
    column = outer_column(own, ranks)
    mine = [column] + [swap(column, ranks, step) for step in range(1, INNER)]
    theirs = []
    for piece in mine:
        theirs.append(lax.ppermute(piece, "tp", [(rank, rank ^ 1) for rank in range(others)]))
    return mine, theirs


PARTS = 4


def project_kernel(groups, *refs):
    mine, theirs, refs = refs[:INNER], refs[INNER : 2 * INNER], refs[2 * INNER :]
    normed, key_cot, value_cot, whole_out, home, *aways = refs[: 5 + INNER - 1]
    tokens, cots, upper, whole, partial, home_buf, away_buf, token_sem, cot_sem, give_sem = refs[5 + INNER - 1 :]
    height = tokens.shape[0] // PARTS
    key_cols = key_cot.shape[1]
    loads = [
        pltpu.make_async_copy(
            normed.at[pl.ds(part * height, height)], tokens.at[pl.ds(part * height, height)], token_sem.at[part]
        )
        for part in range(PARTS)
    ]
    for load in loads:
        load.start()
    cot_loads = [
        pltpu.make_async_copy(key_cot, cots.at[:, pl.ds(0, key_cols)], cot_sem.at[0]),
        pltpu.make_async_copy(value_cot, cots.at[:, pl.ds(key_cols, value_cot.shape[1])], cot_sem.at[1]),
    ]
    for load in cot_loads:
        load.start()
    me, core = lax.axis_index("fs"), lax.axis_index("tp") % 2
    half = mine[0].shape[1]
    rows = mine[0].shape[0] // groups
    for first in range(2):

        @pl.when(core == first)
        def _(first=first):
            for away in range(INNER):
                for group in range(groups):
                    spot = pl.ds(pl.multiple_of((me ^ (group * INNER + away)) * rows, rows), rows)
                    part = slice(group * rows, (group + 1) * rows)
                    whole[spot, first * half : (first + 1) * half] = mine[away][part, :]
                    whole[spot, (1 - first) * half : (2 - first) * half] = theirs[away][part, :]

    gives = [pltpu.make_async_copy(whole, whole_out, give_sem.at[INNER])]
    gives[0].start()
    for part in range(PARTS):
        loads[part].wait()
        span = slice(part * height, (part + 1) * height)
        upper[span, :] = jnp.dot(tokens[span, :], whole[...], preferred_element_type=jnp.float32).astype(jnp.bfloat16)
    for load in cot_loads:
        load.wait()
    partial[...] = lax.dot_general(
        upper[...], cots[...], (((0,), (0,)), ((), ())), preferred_element_type=jnp.float32
    )
    if len(home.shape) == 2:
        gives.append(pltpu.make_async_copy(partial, home, give_sem.at[0]))
        gives[-1].start()
    else:
        low_rows = home.shape[1]
        for away in reversed(range(INNER)):
            for group in range(home.shape[0]):
                slot = group * INNER + ((me % INNER) ^ away)
                block = partial[pl.ds(pl.multiple_of(slot * low_rows, low_rows), low_rows), :]
                if away:
                    away_buf[away - 1, group] = block.astype(jnp.bfloat16)
                else:
                    home_buf[group] = block
            source, target = (away_buf.at[away - 1], aways[away - 1]) if away else (home_buf, home)
            gives.append(pltpu.make_async_copy(source, target, give_sem.at[away]))
            gives[-1].start()
    for give in gives:
        give.wait()


def project(mine, theirs, normed, key_cot, value_cot, me, ranks):
    depth = 2 * mine[0].shape[1]
    groups = ranks // INNER
    low_rows = depth // ranks
    cols = key_cot.shape[1] + value_cot.shape[1]
    local = pl.BlockSpec(memory_space=pltpu.VMEM)
    anywhere = pl.BlockSpec(memory_space=pl.ANY)
    tidy = low_rows % 8 == 0
    home = jax.ShapeDtypeStruct((groups, low_rows, cols) if tidy else (depth, cols), jnp.float32)
    away = jax.ShapeDtypeStruct((groups, low_rows, cols) if tidy else (8, 128), jnp.bfloat16)
    whole, home, *aways = pl.pallas_call(
        functools.partial(project_kernel, groups),
        in_specs=[local] * (2 * INNER) + [anywhere] * 3,
        out_specs=[anywhere] * 2 + [anywhere if tidy else local] * (INNER - 1),
        out_shape=[jax.ShapeDtypeStruct((normed.shape[1], depth), jnp.bfloat16), home] + [away] * (INNER - 1),
        scratch_shapes=[
            pltpu.VMEM(normed.shape, jnp.bfloat16),
            pltpu.VMEM((normed.shape[0], cols), jnp.bfloat16),
            pltpu.VMEM((normed.shape[0], depth), jnp.bfloat16),
            pltpu.VMEM((normed.shape[1], depth), jnp.bfloat16),
            pltpu.VMEM((depth, cols), jnp.float32),
            pltpu.VMEM((groups, low_rows, cols), jnp.float32),
            pltpu.VMEM((INNER - 1, groups, low_rows, cols), jnp.bfloat16),
            pltpu.SemaphoreType.DMA((PARTS,)),
            pltpu.SemaphoreType.DMA((2,)),
            pltpu.SemaphoreType.DMA((INNER + 1,)),
        ],
        name="project",
    )(*in_vmem(*mine, *theirs), normed, key_cot, value_cot)
    if not tidy:
        blocks = home.reshape(groups, INNER, low_rows, cols)
        inner = me % INNER
        home = lax.dynamic_index_in_dim(blocks, inner, 1, keepdims=False)
        aways = [
            lax.dynamic_index_in_dim(blocks, inner ^ step, 1, keepdims=False).astype(jnp.bfloat16)
            for step in range(1, INNER)
        ]
    return whole, home, aways


def scatter_sum(total, aways, me, ranks):
    groups = ranks // INNER
    for step, away in enumerate(aways, 1):
        total = total + swap(away, ranks, step).astype(jnp.float32)
    high = me // INNER
    own = lax.dynamic_index_in_dim(total, high, 0, keepdims=False)
    for step in range(1, groups):
        away = lax.dynamic_index_in_dim(total, high ^ step, 0, keepdims=False).astype(jnp.bfloat16)
        own = own + swap(away, ranks, step * INNER).astype(jnp.float32)
    return own


def pair_sum(parts):
    while len(parts) > 1:
        parts = [left + right for left, right in zip(parts[::2], parts[1::2])]
    return parts[0]


def sum_everywhere(rows_of, ranks):
    value = pair_sum([jnp.sum((part * part).reshape(part.shape[0], -1, 128), axis=1) for part in rows_of])
    received = [swap(value, ranks, step) for step in range(1, INNER)]
    value = pair_sum([value] + received)
    others = lax.axis_size("tp")
    total = value
    for step in range(1, others):
        total = total + lax.ppermute(value, "tp", [(rank, (rank + step) % others) for rank in range(others)])
    return jnp.sum(total)


def copy_kernel(layout, with_own, inherited, resident, *refs):
    count = sum(len(parts) for _, parts in layout)
    basis, directions, *rest = refs
    pieces, rest = rest[:count], rest[count:]
    masters, rest = (rest[:2], rest[2:]) if with_own else ((), rest)
    rest = rest[inherited:]
    copy_key, copy_value, *rest = rest
    results, rest = (rest[:4], rest[4:]) if with_own else ((), rest)
    taken, made, step, take_sem, copy_sem, *rest = rest
    rows = step.shape[0] // INNER
    key_cols = copy_key.shape[1]
    here = lax.axis_index("fs")
    inner = here % INNER
    outer = here // INNER
    takes = []
    if not resident:
        takes = [
            pltpu.make_async_copy(piece, taken.at[slot, pl.ds(0, piece.shape[0])], take_sem.at[slot])
            for slot, piece in enumerate(pieces)
        ]
    for take in takes:
        take.start()
    if with_own:
        own_key, own_value, own_step, own_take, own_give = rest
        own_takes = [
            pltpu.make_async_copy(masters[0], own_key, own_take.at[0]),
            pltpu.make_async_copy(masters[1], own_value, own_take.at[1]),
        ]
        for take in own_takes:
            take.start()
    gives = []
    slot = 0
    blocks = step.shape[1] // key_cols
    for chunk, parts in layout:
        first_row = pl.multiple_of((outer ^ chunk) * INNER * rows, INNER * rows)
        own_spot = pl.ds(pl.multiple_of(inner * rows, rows), rows)
        if with_own and chunk == 0:
            for take in own_takes:
                take.wait()
        for block in range(blocks):
            columns = pl.ds(block * key_cols, key_cols)
            step[:, columns] = jnp.dot(
                basis[pl.ds(first_row, INNER * rows), :], directions[:, columns], preferred_element_type=jnp.float32
            )
            for index, (away, start) in enumerate(parts, slot):
                size = pieces[index].shape[0]
                spot = pl.multiple_of((inner ^ away) * rows + start, size)
                if takes:
                    if block == 0:
                        takes[index].wait()
                    piece = taken[index, pl.ds(0, size), columns]
                else:
                    piece = pieces[index][:, columns]
                change = learn_rate * step[pl.ds(spot, size), columns]
                made[index, pl.ds(0, size), columns] = (piece.astype(jnp.float32) - change).astype(jnp.bfloat16)
                target = pl.ds(pl.multiple_of(first_row + spot, size), size)
                goal = copy_value.at[target, pl.ds((block - 1) * key_cols, key_cols)] if block else copy_key.at[target, :]
                give = pltpu.make_async_copy(
                    made.at[index, pl.ds(0, size), columns], goal, copy_sem.at[index, block]
                )
                give.start()
                gives.append(give)
            if with_own and chunk == 0:
                change = step[own_spot, columns]
                own_step[:, columns] = change
                if block:
                    part = pl.ds((block - 1) * key_cols, key_cols)
                    own_value[:, part] = own_value[:, part] - learn_rate * change
                else:
                    own_key[...] = own_key[...] - learn_rate * change
        slot += len(parts)
        if with_own and chunk == 0:
            value_cols = step.shape[1] - key_cols
            for place_in, (source, target) in enumerate(
                (
                    (own_step.at[:, pl.ds(0, key_cols)], results[0]),
                    (own_step.at[:, pl.ds(key_cols, value_cols)], results[1]),
                    (own_key, results[2]),
                    (own_value, results[3]),
                )
            ):
                give = pltpu.make_async_copy(source, target, own_give.at[place_in])
                give.start()
                gives.append(give)
    for give in gives:
        give.wait()


def write_copies(chunks, masters, basis, directions, key_cols, ranks, earlier, resident):
    rows = basis.shape[0] // ranks
    cols = directions.shape[1]
    layout = tuple((chunk, tuple((away, start) for away, start, _ in parts)) for chunk, parts in chunks)
    pieces = [part for _, parts in chunks for _, _, part in parts]
    count = len(pieces)
    tallest = max(piece.shape[0] for piece in pieces)
    anywhere = pl.BlockSpec(memory_space=pl.ANY)
    local = pl.BlockSpec(memory_space=pltpu.VMEM)
    out_shape = [
        jax.ShapeDtypeStruct((ranks * rows, key_cols), jnp.bfloat16),
        jax.ShapeDtypeStruct((ranks * rows, cols - key_cols), jnp.bfloat16),
    ]
    scratch = [
        pltpu.VMEM((count, tallest, cols), jnp.bfloat16),
        pltpu.VMEM((count, tallest, cols), jnp.bfloat16),
        pltpu.VMEM((INNER * rows, cols), jnp.float32),
        pltpu.SemaphoreType.DMA((count,)),
        pltpu.SemaphoreType.DMA((count, cols // key_cols)),
    ]
    if masters:
        out_shape += [jax.ShapeDtypeStruct(master.shape, jnp.float32) for master in (*masters, *masters)]
        scratch += [
            pltpu.VMEM(masters[0].shape, jnp.float32),
            pltpu.VMEM(masters[1].shape, jnp.float32),
            pltpu.VMEM((rows, cols), jnp.float32),
            pltpu.SemaphoreType.DMA((2,)),
            pltpu.SemaphoreType.DMA((4,)),
        ]
    first_alias = 2 + count + len(masters)
    return pl.pallas_call(
        functools.partial(copy_kernel, layout, bool(masters), len(earlier), resident),
        in_specs=[local, local]
        + [local if resident else anywhere] * count
        + [anywhere] * (len(masters) + len(earlier)),
        out_specs=[anywhere] * len(out_shape),
        out_shape=out_shape,
        scratch_shapes=scratch,
        input_output_aliases={first_alias: 0, first_alias + 1: 1} if earlier else {},
    )(basis, *in_vmem(directions), *(in_vmem(*pieces) if resident else pieces), *masters, *earlier)


def on_device(
    total_count,
    ranks,
    normed,
    key_cot,
    value_cot,
    basis,
    master_key,
    master_value,
    first_key,
    second_key,
    first_value,
    second_value,
):
    me = lax.axis_index("fs")
    key_cols = key_cot.shape[1]
    mine, theirs = gather_basis(basis, ranks)
    master, moments_sent = prepare(master_key, master_value, first_key, second_key, first_value, second_value)
    chunks = spread(master, ranks)
    moments = outer_column(moments_sent, ranks).astype(jnp.float32)
    whole_basis, home, aways = project(mine, theirs, normed, key_cot, value_cot, me, ranks)
    low = scatter_sum(home, aways, me, ranks)
    low_column = outer_column(low.astype(jnp.bfloat16), ranks).astype(jnp.float32)
    height = low.shape[0]
    squares = sum_everywhere(
        [low_column[start : start + height] for start in range(0, low_column.shape[0], height)], ranks
    )
    grad_scale = 1.0 / jnp.sqrt(squares / total_count + norm_eps)

    def advance(low_part, first, second):
        scaled = low_part * grad_scale
        new_first = beta_first * first + (1.0 - beta_first) * scaled
        new_second = beta_second * second + (1.0 - beta_second) * scaled * scaled
        return new_first, new_second

    cols = low.shape[1]
    new_first, new_second = advance(low_column, moments[:, :cols], moments[:, cols:])
    direction = (new_first / (jnp.sqrt(new_second) + epsilon)).astype(jnp.bfloat16)
    directions = inner_gather(direction, me, ranks, low.shape[0])
    first_key, second_key, first_value, second_value, low = lax.optimization_barrier(
        (first_key, second_key, first_value, second_value, low)
    )
    new_first_key, new_second_key = advance(low[:, :key_cols], first_key, second_key)
    new_first_value, new_second_value = advance(low[:, key_cols:], first_value, second_value)
    copy_key, copy_value, *own = write_copies(
        chunks[:-2], (master_key, master_value), whole_basis, directions, key_cols, ranks, (), False
    )
    for name, some in (("middle", chunks[-2:-1]), ("late", chunks[-1:])):
        copy_key, copy_value = write_copies(
            some, (), whole_basis, directions, key_cols, ranks, (copy_key, copy_value), name == "late"
        )
    return (*own, copy_key, copy_value, new_first_key, new_second_key, new_first_value, new_second_value)


def solution(mesh):
    split = P("fs", "tp")
    rows = P("fs", None)
    ranks = mesh.shape["fs"]
    tensor = mesh.shape["tp"]

    def body(*arguments):
        first_key, first_value = arguments[6], arguments[8]
        count = ranks * tensor * (first_key.size + first_value.size)
        return on_device(count, ranks, *arguments)

    return jax.shard_map(
        body,
        mesh=mesh,
        in_specs=(rows, split, split, rows) + (split,) * 6,
        out_specs=(split,) * 4 + (P(None, "tp"),) * 2 + (split,) * 4,
        check_vma=False,
    )
```
